32 devices in a mesh: sp: 8 (over z, x), tp: 4 (over y, core).
Axes of the slice: x: 2, y: 2, z: 4, core: 2. Of those that a mesh axis runs over, the one named last changes fastest.
Arguments:
- inputs: bfloat16 [4096, 2048], P(('sp', 'tp')), may hold values from -6 to 6
- norm_gain: float32 [2048], replicated, may hold values from 0.1 to 1.9
- w_query: bfloat16 [2048, 1024], P(None, 'tp'), may hold values from -1 to 1
- w_key: bfloat16 [2048, 1024], P(None, 'tp'), may hold values from -1 to 1
- w_value: bfloat16 [2048, 1024], P(None, 'tp'), may hold values from -0.125 to 0.125
- query_gain: float32 [2, 64], replicated, may hold values from 1 to 5.5
- key_gain: float32 [2, 64], replicated, may hold values from 1 to 5.5
- lambdas: float32 [8], P('tp'), may hold values from 0.3 to 0.8
- sub_gain: float32 [128], replicated, may hold values from 0.1 to 1.9
- w_gate_b: bfloat16 [2048, 1024], P(None, 'tp'), may hold values from -0.125 to 0.125
- w_gate_c: bfloat16 [2048, 1024], P(None, 'tp'), may hold values from -0.125 to 0.125
- w_conv_in: bfloat16 [2048, 1024], P(None, 'tp'), may hold values from -0.125 to 0.125
- conv_taps: float32 [3, 1024], P(None, 'tp'), may hold values from -3 to 3
- conv_gain: float32 [1024], P('tp'), may hold values from 0.1 to 1.9
- w_out_att: bfloat16 [1024, 2048], P('tp'), may hold values from -0.125 to 0.125
- w_out_conv: bfloat16 [1024, 2048], P('tp'), may hold values from -0.125 to 0.125
Outputs:
- mixed: float32 [4096, 2048], P(('sp', 'tp'))
- log_sums: float32 [8, 2, 4096], P('tp', None, 'sp')
The draws below stay inside these ranges and needn't reach their ends.
All inputs are finite; a program needn't handle non-finite values.
Results may differ from the reference program's by a relative error of at most 0.034.
Values may be sent and summed in bfloat16 or wider, within the bound.
No kernel may reach another device: no remote copies, remote signals or barrier semaphores. Data moves between devices by JAX's collectives and lax.ppermute only.
A program may use at most 192 MiB of HBM per device.

```python
import math
import jax
import jax.numpy as jnp
from jax import lax

D = 2048
ATT_HEADS = 8
QK = 64
VD = 128
CONV = 1024
GROUP = 64
KW = 3
TOKENS = 4096


def draw_query_gain(key, part):
    spread = jax.random.uniform(jax.random.fold_in(key, 11), (2, QK), jnp.float32, -1.0, 1.0)
    return 1.3 * (1.0 + 0.2 * spread)


def draw_key_gain(key, part):
    spread = jax.random.uniform(jax.random.fold_in(key, 23), (2, QK), jnp.float32, -1.0, 1.0)
    return 1.3 * (1.0 + 0.2 * spread)


def projection_pair(key):
    first = jax.random.normal(jax.random.fold_in(key, 101), (D, ATT_HEADS * 2 * QK), jnp.float32)
    second = jax.random.normal(jax.random.fold_in(key, 103), (D, ATT_HEADS * 2 * QK), jnp.float32)
    scale = D ** (-0.5)
    return (jnp.clip(first, -5.0, 5.0) * scale, jnp.clip(second, -5.0, 5.0) * scale)


def draw_w_query(key, part):
    first, second = projection_pair(key)
    return first.astype(jnp.bfloat16)


def draw_w_key(key, part):
    first, second = projection_pair(key)
    return second.astype(jnp.bfloat16)


def draw_inputs(key, part):
    base = jax.random.normal(jax.random.fold_in(key, 201), (TOKENS, D), jnp.float32)
    return jnp.clip(base, -6.0, 6.0).astype(jnp.bfloat16)


def block_levels(own_key, shape, pieces, low, high):
    loudness = 1.0
    for dim, shards_of in pieces:
        draws = jax.random.uniform(jax.random.fold_in(jax.random.fold_in(own_key, 6), dim), (shards_of,), jnp.float32, low / len(pieces), high / len(pieces))
        loudness = loudness * jnp.repeat(jnp.exp(draws), shape[dim] // shards_of).reshape((-1,) + (1,) * (len(shape) - 1 - dim))
    return loudness


def scatter_about(key, shape, deviation, reach, cuts=(), held_as=jnp.bfloat16):
    array = jax.random.normal(key, shape, jnp.float32) * deviation
    if len(cuts) > 0:
        array = block_levels(key, shape, cuts, -0.22, 0.18) * array
    return jnp.clip(array, min=-reach, max=reach).astype(held_as)


def setup_inputs(seed: int = 0) -> dict:
    key_list = jax.random.split(jax.random.key(seed), 17)
    inputs = draw_inputs(jax.random.fold_in(key_list[16], 71), 0)
    norm_gain = jnp.clip(1.0 + 0.18 * jax.random.normal(key_list[1], (D,), jnp.float32), 0.1, 1.9)
    w_query = draw_w_query(jax.random.fold_in(key_list[16], 71), 0)
    w_key = draw_w_key(jax.random.fold_in(key_list[16], 71), 0)
    w_value = scatter_about(key_list[4], (D, ATT_HEADS * VD), D ** -0.5, 0.125, ((1, 4),))
    query_gain = draw_query_gain(jax.random.fold_in(key_list[16], 71), 0)
    key_gain = draw_key_gain(jax.random.fold_in(key_list[16], 71), 0)
    lambdas = jnp.clip(0.3 + 0.5 * jax.random.uniform(key_list[7], (ATT_HEADS,), jnp.float32) ** block_levels(key_list[7], (ATT_HEADS,), ((0, 4),), -0.2, 0.2), 0.3, 0.8)
    sub_gain = jnp.clip(1.0 + 0.18 * jax.random.normal(key_list[8], (VD,), jnp.float32), 0.1, 1.9)
    w_gate_b = scatter_about(key_list[9], (D, CONV), D ** -0.5, 0.125, ((1, 4),))
    w_gate_c = scatter_about(key_list[10], (D, CONV), D ** -0.5, 0.125, ((1, 4),))
    w_conv_in = scatter_about(key_list[11], (D, CONV), D ** -0.5, 0.125, ((1, 4),))
    conv_taps = scatter_about(key_list[12], (KW, CONV), 0.577, 3.0, ((1, 4),), jnp.float32)
    conv_gain = jnp.clip(1.0 + 0.18 * jax.random.normal(key_list[13], (CONV,), jnp.float32), 0.1, 1.9)
    w_out_att = scatter_about(key_list[14], (ATT_HEADS * VD, D), (ATT_HEADS * VD + CONV) ** -0.5, 0.125, ((0, 4),))
    w_out_conv = scatter_about(key_list[15], (CONV, D), (ATT_HEADS * VD + CONV) ** -0.5, 0.125, ((0, 4),))
    return {"inputs": inputs, "norm_gain": norm_gain, "w_query": w_query, "w_key": w_key, "w_value": w_value, "query_gain": query_gain, "key_gain": key_gain, "lambdas": lambdas, "sub_gain": sub_gain, "w_gate_b": w_gate_b, "w_gate_c": w_gate_c, "w_conv_in": w_conv_in, "conv_taps": conv_taps, "conv_gain": conv_gain, "w_out_att": w_out_att, "w_out_conv": w_out_conv}


eps = 1e-06

def rms_scale(values):
    return values * lax.rsqrt(lax.optimization_barrier(jnp.mean(values * values, axis=-1, keepdims=True)) + eps)

def rounded(values):
    return lax.optimization_barrier(values.astype(jnp.bfloat16)).astype(jnp.float32)

def reference(inputs, norm_gain, w_query, w_key, w_value, query_gain, key_gain, lambdas, sub_gain, w_gate_b, w_gate_c, w_conv_in, conv_taps, conv_gain, w_out_att, w_out_conv):
    length = inputs.shape[0]
    normed = (rms_scale(inputs.astype(jnp.float32)) * norm_gain).astype(jnp.bfloat16)

    def project(weight):
        return jnp.dot(normed, weight, preferred_element_type=jnp.float32).astype(jnp.bfloat16)
    query = project(w_query).reshape(length, ATT_HEADS, 2, QK)
    key = project(w_key).reshape(length, ATT_HEADS, 2, QK)
    value = project(w_value).reshape(length, ATT_HEADS, VD)
    qn = (rms_scale(query.astype(jnp.float32)) * query_gain * QK ** (-0.5)).astype(jnp.bfloat16)
    kn = (rms_scale(key.astype(jnp.float32)) * key_gain).astype(jnp.bfloat16)
    keys_f = kn.astype(jnp.float32)
    values_f = value.astype(jnp.float32)
    qblock = math.gcd(length, 128)
    key_pos = jnp.arange(length, dtype=jnp.int32)

    def one_block(start):
        qrows = lax.dynamic_slice_in_dim(qn, start, qblock, 0).astype(jnp.float32)
        scores = jnp.einsum('qhmd,khmd->hmqk', qrows, keys_f)
        query_pos = start + jnp.arange(qblock, dtype=jnp.int32)
        allowed = key_pos[None, :] <= query_pos[:, None]
        scores = jnp.where(allowed, scores, -1e+30)
        top = lax.optimization_barrier(jnp.max(scores, axis=-1, keepdims=True))
        prob = jnp.where(allowed, jnp.exp(scores - top), 0.0)
        total = lax.optimization_barrier(jnp.sum(prob, axis=-1))
        acc = jnp.einsum('hmqk,khd->hmqd', rounded(prob), values_f)
        return (acc / total[..., None], top[..., 0] + jnp.log(total))
    starts = (jnp.arange(length // qblock) * qblock).astype(jnp.int32)
    outs, logs = lax.map(one_block, starts)
    map_out = outs.transpose(1, 2, 0, 3, 4).reshape(ATT_HEADS, 2, length, VD)
    attn = map_out[:, 0] - lambdas[:, None, None] * map_out[:, 1]
    heads_out = (rms_scale(attn) * sub_gain).astype(jnp.bfloat16)
    heads_out = heads_out.transpose(1, 0, 2).reshape(length, ATT_HEADS * VD)
    log_sums = logs.transpose(1, 2, 0, 3).reshape(ATT_HEADS, 2, length)
    gate_b = project(w_gate_b).astype(jnp.float32)
    gate_c = project(w_gate_c).astype(jnp.float32)
    conv_in = project(w_conv_in).astype(jnp.float32)
    u_vals = rounded(gate_c * conv_in)
    padded = jnp.concatenate([jnp.zeros((KW - 1, CONV), jnp.float32), u_vals], axis=0)
    conv = jnp.zeros((length, CONV), jnp.float32)
    for tap in range(KW):
        conv = conv + conv_taps[tap] * padded[tap:tap + length]
    gated = gate_b * conv
    grouped = rms_scale(gated.reshape(length, CONV // GROUP, GROUP)).reshape(length, CONV)
    conv_out = (grouped * conv_gain).astype(jnp.bfloat16)
    mixed = jnp.dot(heads_out, w_out_att, preferred_element_type=jnp.float32)
    mixed = mixed + jnp.dot(conv_out, w_out_conv, preferred_element_type=jnp.float32)
    return (mixed, log_sums)
```

```python
import functools
import math

import jax
import jax.numpy as jnp
from jax import lax
from jax.experimental import pallas as pl
from jax.experimental.pallas import tpu as pltpu
from jax.sharding import PartitionSpec as P

GROUP = 64
eps = 1e-06
LOG2E = math.log2(math.e)
LN2 = math.log(2.0)


F32 = jnp.float32
BF16 = jnp.bfloat16


def swap(shard, axis, bit):
    count = lax.axis_size(axis)
    return lax.ppermute(shard, axis, [(i, i ^ bit) for i in range(count)])


def from_behind(shard, axis, by):
    count = lax.axis_size(axis)
    pairs = [(i, i + by) for i in range(count) if 0 <= i + by < count]
    return lax.ppermute(shard, axis, pairs)


def rms_scale(values):
    return values * lax.rsqrt(jnp.mean(values * values, axis=-1, keepdims=True) + eps)


def dot(a, b):
    return jnp.dot(a, b, preferred_element_type=F32)


def proj_body(idx_ref, x_ref, gain_ref, wq_ref, wk_ref, wv_ref, qg_ref, kg_ref,
              own_ref, oth_ref, xn_ref, *, comp):
    j = pl.program_id(0)
    width = qg_ref.shape[1]

    @pl.when(j == 0)
    def _():
        xf = x_ref[...].astype(F32)
        ms = jnp.mean(xf * xf, axis=-1, keepdims=True)
        xn_ref[...] = (xf * lax.rsqrt(ms + eps) * gain_ref[...]).astype(BF16)

    xn = xn_ref[...]
    row = lax.broadcasted_iota(jnp.int32, (width, width), 0) // comp
    col = lax.broadcasted_iota(jnp.int32, (width, width), 1) // comp
    block = jnp.where(row == col, 1.0, 0.0).astype(BF16)

    def head_norm(w_ref, g_ref):
        val = dot(xn, w_ref[...]).astype(BF16).astype(F32)
        sq = val * val
        hi = sq.astype(BF16)
        lo = (sq - hi.astype(F32)).astype(BF16)
        ms = (dot(hi, block) + dot(lo, block)) * (1.0 / comp)
        return (val * lax.rsqrt(ms + eps) * g_ref[...]).astype(BF16)

    def put(first, ref):
        @pl.when(j == first)
        def _():
            ref[...] = head_norm(wq_ref, qg_ref)

        @pl.when(j == first + 1)
        def _():
            ref[...] = head_norm(wk_ref, kg_ref)

        @pl.when(j == first + 2)
        def _():
            ref[...] = dot(xn, wv_ref[...]).astype(BF16)

    put(0, own_ref)
    put(3, oth_ref)


def project(xbit, x, gain, wq, wk, wv, qgain, kgain, comp):
    rows, d = x.shape
    width = wq.shape[1] // 2

    def wspec(t):
        def index(j, s):
            second = jnp.where(j > t, 1, 0)
            return (0, second ^ s[0])

        return pl.BlockSpec((d, width), index)

    full = lambda shape: pl.BlockSpec(shape, lambda j, s: (0,) * len(shape))
    return pl.pallas_call(
        functools.partial(proj_body, comp=comp),
        out_shape=(
            jax.ShapeDtypeStruct((rows, 3 * width), BF16),
            jax.ShapeDtypeStruct((rows, 3 * width), BF16),
            jax.ShapeDtypeStruct((rows, d), BF16),
        ),
        grid_spec=pltpu.PrefetchScalarGridSpec(
            num_scalar_prefetch=1,
            grid=(6,),
            in_specs=[
                full((rows, d)),
                full((1, d)),
                wspec(0),
                wspec(1),
                wspec(2),
                full((1, width)),
                full((1, width)),
            ],
            out_specs=(
                pl.BlockSpec((rows, width), lambda j, s: (0, jnp.minimum(j, 2))),
                pl.BlockSpec((rows, width), lambda j, s: (0, jnp.maximum(j - 3, 0))),
                full((rows, d)),
            ),
        ),
        name="proj",
    )(xbit, x, gain, wq, wk, wv, qgain, kgain)


def scores(k, q):
    return lax.dot_general(k, q, (((1,), (1,)), ((), ())), preferred_element_type=F32)


def diag_body(base_ref, *refs, comp, rows):
    chunks = refs[:4]
    q_ref, o_ref, m_ref, l_ref, k_scr, vt_scr = refs[4:]
    width = q_ref.shape[1]
    for g in range(4):
        start = pl.multiple_of(base_ref[g], rows)
        q_ref[pl.ds(start, rows), :] = chunks[g][:, :width]
        k_scr[pl.ds(start, rows), :] = chunks[g][:, width : 2 * width]
        vt_scr[:, pl.ds(start, rows)] = chunks[g][:, 2 * width :].T
    keep = lax.broadcasted_iota(jnp.int32, (rows, rows), 0) <= lax.broadcasted_iota(
        jnp.int32, (rows, rows), 1
    )
    for t in range(4):
        qs = slice(t * rows, (t + 1) * rows)
        for mi in range(2):
            cs = slice(mi * comp, (mi + 1) * comp)
            q = q_ref[qs, cs]
            sd = jnp.where(keep, scores(k_scr[qs, cs], q), -1e30)
            top = jnp.max(sd, axis=0, keepdims=True)
            if t > 0:
                sf = scores(k_scr[: t * rows, cs], q)
                top = jnp.maximum(top, jnp.max(sf, axis=0, keepdims=True))
            pd = jnp.exp2(sd - top)
            total = jnp.sum(pd, axis=0, keepdims=True)
            out = dot(vt_scr[:, qs], pd.astype(BF16))
            if t > 0:
                pf = jnp.exp2(sf - top)
                total = total + jnp.sum(pf, axis=0, keepdims=True)
                out = out + dot(vt_scr[:, : t * rows], pf.astype(BF16))
            o_ref[mi, :, qs] = out
            m_ref[mi : mi + 1, qs] = top
            l_ref[mi : mi + 1, qs] = total


def diagonal(bases, chunks, comp):
    rows, three = chunks[0].shape
    width = three // 3
    n = 4 * rows
    full = lambda shape: pl.BlockSpec(shape, lambda i, s: (0,) * len(shape))
    return pl.pallas_call(
        functools.partial(diag_body, comp=comp, rows=rows),
        out_shape=(
            jax.ShapeDtypeStruct((n, width), BF16),
            jax.ShapeDtypeStruct((2, width, n), F32),
            jax.ShapeDtypeStruct((2, n), F32),
            jax.ShapeDtypeStruct((2, n), F32),
        ),
        grid_spec=pltpu.PrefetchScalarGridSpec(
            num_scalar_prefetch=1,
            grid=(1,),
            in_specs=[full((rows, three))] * 4,
            out_specs=(full((n, width)), full((2, width, n)), full((2, n)), full((2, n))),
            scratch_shapes=[pltpu.VMEM((n, width), BF16), pltpu.VMEM((width, n), BF16)],
        ),
        name="diag",
    )(bases, *chunks)


def hop_body(flag_ref, q_ref, kv_ref, oi_ref, mi_ref, li_ref, o_ref, m_ref, l_ref, *, comp, tile):
    n, width = q_ref.shape

    @pl.when(flag_ref[0] > 0)
    def _():
        vt = kv_ref[:, width:].T
        for t in range(n // tile):
            qs = slice(t * tile, (t + 1) * tile)
            for mi in range(2):
                cs = slice(mi * comp, (mi + 1) * comp)
                s = scores(kv_ref[:, cs], q_ref[qs, cs])
                old = mi_ref[mi : mi + 1, qs]
                top = jnp.maximum(old, jnp.max(s, axis=0, keepdims=True))
                p = jnp.exp2(s - top)
                alpha = jnp.exp2(old - top)
                l_ref[mi : mi + 1, qs] = li_ref[mi : mi + 1, qs] * alpha + jnp.sum(
                    p, axis=0, keepdims=True
                )
                m_ref[mi : mi + 1, qs] = top
                o_ref[mi, :, qs] = oi_ref[mi, :, qs] * alpha + dot(vt, p.astype(BF16))

    @pl.when(flag_ref[0] <= 0)
    def _():
        o_ref[...] = oi_ref[...]
        m_ref[...] = mi_ref[...]
        l_ref[...] = li_ref[...]


def absorb(flag, q, kv, state, comp):
    o, m, l = state
    full = lambda shape: pl.BlockSpec(shape, lambda i, s: (0,) * len(shape))
    return pl.pallas_call(
        functools.partial(hop_body, comp=comp, tile=256),
        out_shape=tuple(jax.ShapeDtypeStruct(a.shape, a.dtype) for a in state),
        grid_spec=pltpu.PrefetchScalarGridSpec(
            num_scalar_prefetch=1,
            grid=(1,),
            in_specs=[full(q.shape), full(kv.shape), full(o.shape), full(m.shape), full(l.shape)],
            out_specs=(full(o.shape), full(m.shape), full(l.shape)),
        ),
        input_output_aliases={3: 0, 4: 1, 5: 2},
        name="hop",
    )(flag, q, kv, o, m, l)


def finish_body(lam_ref, o_ref, m_ref, l_ref, gain_ref, h_ref, lse_ref):
    n = h_ref.shape[0]
    tile = n // 4
    for t in range(4):
        qs = slice(t * tile, (t + 1) * tile)
        attn = o_ref[0, :, qs] / l_ref[0:1, qs] - lam_ref[0] * (o_ref[1, :, qs] / l_ref[1:2, qs])
        ms = jnp.mean(attn * attn, axis=0, keepdims=True)
        h_ref[qs, :] = (attn * lax.rsqrt(ms + eps) * gain_ref[...]).T.astype(BF16)
    lse_ref[...] = m_ref[...] * LN2 + jnp.log(l_ref[...])


def finish(lam, state, gain):
    o, m, l = state
    full = lambda shape: pl.BlockSpec(shape, lambda i: (0,) * len(shape))
    return pl.pallas_call(
        finish_body,
        out_shape=(
            jax.ShapeDtypeStruct((o.shape[2], o.shape[1]), BF16),
            jax.ShapeDtypeStruct(m.shape, F32),
        ),
        grid=(1,),
        in_specs=[
            pl.BlockSpec(memory_space=pltpu.SMEM),
            full(o.shape), full(m.shape), full(l.shape), full(gain.shape),
        ],
        out_specs=(full((o.shape[2], o.shape[1])), full(m.shape)),
        name="finish",
    )(lam, o, m, l, gain)


def out_body(tp_ref, h_ref, w0_ref, w1_ref, w2_ref, w3_ref, conv_ref, out_ref):
    half = h_ref.shape[0] // 2
    width = h_ref.shape[2]
    acc = conv_ref[...]
    for r, w_ref in enumerate((w0_ref, w1_ref, w2_ref, w3_ref)):
        for xb in range(2):
            piece = h_ref[xb * half + (tp_ref[0] ^ r)]
            acc = acc + dot(piece, w_ref[xb * width : (xb + 1) * width, :])
    out_ref[...] = acc


def out_project(tp, heads, weights, conv):
    rows, d = conv.shape
    tile = d // 4
    k = weights[0].shape[0]
    wspec = pl.BlockSpec((k, tile), lambda j, s: (0, j))
    return pl.pallas_call(
        out_body,
        out_shape=jax.ShapeDtypeStruct((rows, d), F32),
        grid_spec=pltpu.PrefetchScalarGridSpec(
            num_scalar_prefetch=1,
            grid=(4,),
            in_specs=[
                pl.BlockSpec(heads.shape, lambda j, s: (0, 0, 0)),
                wspec, wspec, wspec, wspec,
                pl.BlockSpec((rows, tile), lambda j, s: (0, j)),
            ],
            out_specs=pl.BlockSpec((rows, tile), lambda j, s: (0, j)),
        ),
        name="outproj",
    )(tp, heads, *weights, conv)


def on_device(
    inputs,
    norm_gain,
    w_query,
    w_key,
    w_value,
    query_gain,
    key_gain,
    lambdas,
    sub_gain,
    w_gate_b,
    w_gate_c,
    w_conv_in,
    conv_taps,
    conv_gain,
    w_out_att,
    w_out_conv,
):
    comp = query_gain.shape[1]
    channels = conv_gain.shape[0]
    taps_count = conv_taps.shape[0]
    piece, d = inputs.shape
    sp_size = lax.axis_size("sp")
    tp_size = lax.axis_size("tp")
    assert tp_size == 4 and lambdas.shape[0] == 2 and sp_size % 2 == 0
    rows = piece * tp_size
    pair = 2 * piece
    depth = sp_size // 2
    sp = lax.axis_index("sp")
    tp = lax.axis_index("tp")
    xbit = sp % 2
    zpos = sp // 2
    core = tp % 2
    ybit = tp // 2

    def one(v):
        return jnp.reshape(v, (1,)).astype(jnp.int32)

    def halves(mine, other):
        return jnp.concatenate(
            [jnp.where(core == 0, mine, other), jnp.where(core == 0, other, mine)], axis=0
        )

    gain_row = norm_gain.reshape(1, d)
    qg = (query_gain.reshape(1, -1) * (comp ** (-0.5) * LOG2E)).astype(F32)
    kg = key_gain.reshape(1, -1)

    far = swap(inputs, "tp", 2)
    near = swap(inputs, "tp", 1)
    x_a = halves(inputs, near)
    own_a, oth_a, xn_a = project(
        one(xbit), x_a, gain_row, w_query, w_key, w_value, qg, kg, comp
    )
    rec_a = swap(oth_a, "sp", 1)
    width = own_a.shape[1] // 3
    kv_a = jnp.concatenate([own_a[:, width:], rec_a[:, width:]], axis=0)

    far_near = swap(far, "tp", 1)
    x_b = halves(far, far_near)
    own_b, oth_b, xn_b = project(
        one(xbit), x_b, gain_row, w_query, w_key, w_value, qg, kg, comp
    )
    rec_b = swap(oth_b, "sp", 1)
    kv_b = jnp.concatenate([own_b[:, width:], rec_b[:, width:]], axis=0)

    base_a = ybit * pair
    base_b = (1 - ybit) * pair
    mine = xbit * rows
    other = (1 - xbit) * rows
    bases = jnp.stack([mine + base_a, other + base_a, mine + base_b, other + base_b]).astype(
        jnp.int32
    )
    q_all, *state = diagonal(bases, (own_a, rec_a, own_b, rec_b), comp)
    state = tuple(state)
    for hop in range(1, depth):
        kv_a = from_behind(kv_a, "sp", 2)
        kv_b = from_behind(kv_b, "sp", 2)
        flag = one(zpos >= hop)
        state = absorb(flag, q_all, kv_a, state, comp)
        state = absorb(flag, q_all, kv_b, state, comp)
    lam = jnp.where(xbit == 0, lambdas[0], lambdas[1]).reshape(1)
    heads, lse = finish(lam, state, sub_gain.reshape(-1, 1))

    lse3 = lse.reshape(2, 2, rows)
    lse_mine = jnp.where(xbit == 0, lse3[:, 0], lse3[:, 1])
    lse_other = swap(jnp.where(xbit == 0, lse3[:, 1], lse3[:, 0]), "sp", 1)
    log_sums = jnp.stack(
        [jnp.where(xbit == 0, lse_mine, lse_other), jnp.where(xbit == 0, lse_other, lse_mine)]
    )

    def conv_dots(weight):
        dot_a = dot(xn_a, weight).astype(BF16)
        dot_b = dot(xn_b, weight).astype(BF16)
        return jnp.concatenate(
            [jnp.where(ybit == 0, dot_a, dot_b), jnp.where(ybit == 0, dot_b, dot_a)], axis=0
        ).astype(F32)

    gate_b = conv_dots(w_gate_b)
    u_vals = (conv_dots(w_gate_c) * conv_dots(w_conv_in)).astype(BF16)
    edge = from_behind(u_vals[rows - (taps_count - 1) :], "sp", 1)
    padded = jnp.concatenate([edge, u_vals], axis=0).astype(F32)
    conv = conv_taps[0] * padded[0:rows]
    for tap in range(1, taps_count):
        conv = conv + conv_taps[tap] * padded[tap : tap + rows]
    gated = gate_b * conv
    grouped = rms_scale(gated.reshape(rows, channels // GROUP, GROUP)).reshape(rows, channels)
    conv_out = (grouped * conv_gain).astype(BF16)
    partial = dot(conv_out, w_out_conv).reshape(2, 2, piece, d)
    kept = jnp.where(core == 0, partial[:, 0], partial[:, 1])
    sent = jnp.where(core == 0, partial[:, 1], partial[:, 0]).astype(BF16)
    kept = kept + swap(sent, "tp", 1).astype(F32)
    conv_mixed = jnp.where(ybit == 0, kept[0], kept[1]) + swap(
        jnp.where(ybit == 0, kept[1], kept[0]).astype(BF16), "tp", 2
    ).astype(F32)

    w_far = swap(w_out_att, "tp", 2)
    weights = (w_out_att, swap(w_out_att, "tp", 1), w_far, swap(w_far, "tp", 1))

    groups = [
        [(z * 2 + x) * tp_size + t for x in range(2) for t in range(tp_size)]
        for z in range(depth)
    ]
    pieces = lax.all_to_all(
        heads.reshape(2 * tp_size, piece, width),
        ("sp", "tp"), 0, 0, axis_index_groups=groups, tiled=True,
    )
    mixed = out_project(one(tp), pieces, weights, conv_mixed)
    return (mixed, log_sums)


def solution(mesh):
    in_specs = (
        P(("sp", "tp"), None),
        P(),
        P(None, "tp"),
        P(None, "tp"),
        P(None, "tp"),
        P(),
        P(),
        P("tp"),
        P(),
        P(None, "tp"),
        P(None, "tp"),
        P(None, "tp"),
        P(None, "tp"),
        P("tp"),
        P("tp", None),
        P("tp", None),
    )
    out_specs = (P(("sp", "tp"), None), P("tp", None, "sp"))
    return jax.shard_map(
        on_device, mesh=mesh, in_specs=in_specs, out_specs=out_specs, check_vma=False
    )
```
